512 devices in a mesh: grp: 2 (over y), fs: 32 (over z), tp: 8 (over x, core).
Axes of the slice: x: 4, y: 2, z: 32, core: 2. Of those that a mesh axis runs over, the one named last changes fastest.
The devices are a block of a 4x8x32 slice.
Arguments:
- layer_input_tokens: bfloat16 [32768, 2048], P(('grp', 'fs')), parts along dimension 0, may hold values from -6 to 6
- attention_norm_gain: float32 [2048], replicated, may hold values from 0.1 to 1.9
- query_projection: bfloat16 [2048, 1024], P('fs', 'tp'), may hold values from -0.125 to 0.125
- key_projection: bfloat16 [2048, 1024], P('fs', 'tp'), may hold values from -0.125 to 0.125
- value_projection: bfloat16 [2048, 2048], P('fs', 'tp'), may hold values from -0.125 to 0.125
- decay_first_factor: bfloat16 [2048, 16], replicated, may hold values from -0.125 to 0.125
- decay_second_factor: bfloat16 [16, 1024], P(None, 'tp'), may hold values from -1.5 to 1.5
- decay_logit_bias: float32 [1024], P('tp'), may hold values from -0.5 to 6
- extra_log_decay: float32 [32768, 8], P(('grp', 'fs'), 'tp'), parts along dimension 0, may hold values from -0.7 to 0
- head_output_gain: float32 [256], replicated, may hold values from 0.1 to 1.9
- attention_output_projection: bfloat16 [2048, 2048], P(('tp', 'fs')), may hold values from -0.125 to 0.125
- feedforward_norm_gain: float32 [2048], replicated, may hold values from 0.1 to 1.9
- gate_projection: bfloat16 [2048, 5632], P('fs', 'tp'), may hold values from -0.125 to 0.125
- up_projection: bfloat16 [2048, 5632], P('fs', 'tp'), may hold values from -0.125 to 0.125
- down_projection: bfloat16 [5632, 2048], P(('tp', 'fs')), may hold values from -0.078125 to 0.078125
Outputs:
- result: bfloat16 [32768, 2048], P(('grp', 'fs')), parts along dimension 0
The draws below stay inside these ranges and needn't reach their ends.
There are 2 independent parts, one for each index of `grp`. The reference program is written for one: setup_inputs(seed, part) draws one part's arguments, and reference() takes and returns one part's arrays. A program takes and returns all parts, laid end to end along the dimension named above; an argument that names none is the same for every part. Nothing has to cross between parts.
All inputs are finite; a program needn't handle non-finite values.
Results may differ from the reference program's by a relative error of at most 0.02.
Values may be sent and summed in bfloat16 or wider, within the bound.
A program may use at most 64 MiB of HBM per device.

```python
import jax
import jax.numpy as jnp
from jax import lax

D = 2048
HEADS = 8
KEY_CHANNELS = 128
DV = 256
RANK = 16
FF = 5632
BLOCK = 64
SEQ_LEN = 512
TOKENS = 16384
N_FS = 32
N_TP = 8


def draw_decay_logit_bias(key, part):
    pick = jax.random.randint(jax.random.fold_in(key, 11), (HEADS * KEY_CHANNELS,), 0, 10)
    fast = jax.random.uniform(jax.random.fold_in(key, 12), (HEADS * KEY_CHANNELS,), jnp.float32, -0.5, 1.0)
    slow = jax.random.uniform(jax.random.fold_in(key, 13), (HEADS * KEY_CHANNELS,), jnp.float32, 3.5, 5.5)
    return jnp.where(pick < 5, fast, slow).astype(jnp.float32)


def draw_extra_log_decay(key, part):
    hits = jax.random.randint(jax.random.fold_in(key, 21), (TOKENS, HEADS), 0, SEQ_LEN)
    depth = jnp.log(jax.random.uniform(jax.random.fold_in(key, 22), (TOKENS, HEADS), jnp.float32, 0.5, 0.8))
    return jnp.where(hits < 3, depth, 0.0).astype(jnp.float32)


def shard_levels(stream_key, extent, cuts, smallest, largest):
    def one(dim, parts):
        steps = jax.random.uniform(jax.random.fold_in(jax.random.fold_in(stream_key, 6), dim), (parts,), jnp.float32, smallest / len(cuts), largest / len(cuts))
        return jnp.repeat(jnp.exp(steps), extent[dim] // parts).reshape((-1,) + (1,) * (len(extent) - dim - 1))

    level = one(*cuts[0])
    for cut in cuts[1:]:
        level = level * one(*cut)
    return level


def noise(own_key, dims, deviation, most, cuts=(), held_as=jnp.bfloat16):
    entries = deviation * jax.random.normal(own_key, dims, jnp.float32)
    if cuts:
        entries = entries * shard_levels(own_key, dims, cuts, -0.22, 0.18)
    return jnp.clip(entries, -most, most).astype(held_as)


def setup_inputs(seed: int = 0, part: int = 0) -> dict:
    seeds = jax.random.split(jax.random.key(seed), 16)
    part_splits = jax.random.split(jax.random.fold_in(seeds[15], part), 16)
    layer_input_tokens = noise(part_splits[0], (TOKENS, D), 1.0, 6.0, ((0, 32),))
    attention_norm_gain = jnp.clip(1.0 + 0.18 * jax.random.normal(seeds[1], (D,), jnp.float32), 0.1, 1.9)
    query_projection = noise(seeds[2], (D, HEADS * KEY_CHANNELS), D ** -0.5, 0.125, ((0, 32), (1, 8)))
    key_projection = noise(seeds[3], (D, HEADS * KEY_CHANNELS), D ** -0.5, 0.125, ((0, 32), (1, 8)))
    value_projection = noise(seeds[4], (D, HEADS * DV), D ** -0.5, 0.125, ((0, 32), (1, 8)))
    decay_first_factor = noise(seeds[5], (D, RANK), D ** -0.5, 0.125)
    decay_second_factor = noise(seeds[6], (RANK, HEADS * KEY_CHANNELS), RANK ** -0.5, 1.5, ((1, 8),))
    decay_logit_bias = draw_decay_logit_bias(jax.random.fold_in(seeds[15], 71), part)
    extra_log_decay = draw_extra_log_decay(jax.random.fold_in(jax.random.fold_in(seeds[15], part), 71), part)
    head_output_gain = jnp.clip(1.0 + 0.18 * jax.random.normal(seeds[9], (DV,), jnp.float32), 0.1, 1.9)
    attention_output_projection = noise(seeds[10], (HEADS * DV, D), (HEADS * DV) ** -0.5, 0.125, ((0, 256),))
    feedforward_norm_gain = jnp.clip(1.0 + 0.18 * jax.random.normal(seeds[11], (D,), jnp.float32), 0.1, 1.9)
    gate_projection = noise(seeds[12], (D, FF), D ** -0.5, 0.125, ((0, 32), (1, 8)))
    up_projection = noise(seeds[13], (D, FF), D ** -0.5, 0.125, ((0, 32), (1, 8)))
    down_projection = noise(seeds[14], (FF, D), FF ** -0.5, 0.078125, ((0, 256),))
    return {"layer_input_tokens": layer_input_tokens, "attention_norm_gain": attention_norm_gain, "query_projection": query_projection, "key_projection": key_projection, "value_projection": value_projection, "decay_first_factor": decay_first_factor, "decay_second_factor": decay_second_factor, "decay_logit_bias": decay_logit_bias, "extra_log_decay": extra_log_decay, "head_output_gain": head_output_gain, "attention_output_projection": attention_output_projection, "feedforward_norm_gain": feedforward_norm_gain, "gate_projection": gate_projection, "up_projection": up_projection, "down_projection": down_projection}


normed_gate = 16.0

def norm_rows(values, gain):
    wide = values.astype(jnp.float32)
    scale = lax.rsqrt(lax.optimization_barrier(jnp.mean(wide * wide, axis=-1, keepdims=True)) + 1e-06)
    return wide * scale * gain

def block_scan(queries, keys, values, decays):
    length, key_channel_width = queries.shape
    value_width = values.shape[1]
    count = length // BLOCK
    lower_mask = jnp.arange(BLOCK)[:, None] >= jnp.arange(BLOCK)[None, :]

    def advance(carry, items):
        query_block, key_block, value_block, decay_block = items
        running = jnp.cumsum(decay_block, axis=0)
        middle = running[BLOCK // 2 - 1]
        closing = running[BLOCK - 1]
        carried = jnp.dot(query_block * jnp.exp(running), carry, precision=lax.Precision.HIGHEST)
        scores = jnp.dot(query_block * jnp.exp(running - middle), (key_block * jnp.exp(middle - running)).T, precision=lax.Precision.HIGHEST)
        scores = jnp.where(lower_mask, scores, 0.0)
        inside = jnp.dot(scores, value_block, precision=lax.Precision.HIGHEST)
        fresh = carry * jnp.exp(closing)[:, None] + jnp.dot((key_block * jnp.exp(closing - running)).T, value_block, precision=lax.Precision.HIGHEST)
        return (fresh, carried + inside)
    items = (queries.reshape(count, BLOCK, key_channel_width), keys.reshape(count, BLOCK, key_channel_width), values.reshape(count, BLOCK, value_width), decays.reshape(count, BLOCK, key_channel_width))
    _, outputs = lax.scan(advance, jnp.zeros((key_channel_width, value_width), jnp.float32), items)
    return outputs.reshape(length, value_width)

def both_ways(queries, keys, values, decays):
    ahead = block_scan(queries, keys, values, decays)
    behind = block_scan(jnp.flip(queries, 0), jnp.flip(keys, 0), jnp.flip(values, 0), jnp.flip(decays, 0))
    return ahead + jnp.flip(behind, 0)

def head_norm(mixed, gain):
    scale = lax.rsqrt(lax.optimization_barrier(jnp.mean(mixed * mixed, axis=-1, keepdims=True)) + 1e-06)
    return mixed * scale * gain

def group_sum(left, right):
    width = left.shape[1] // N_TP
    total = jnp.zeros((left.shape[0], right.shape[1]), jnp.float32)
    for group in range(N_TP):
        part = jnp.dot(left[:, group * width:(group + 1) * width], right[group * width:(group + 1) * width], preferred_element_type=jnp.float32)
        part = lax.optimization_barrier(part.astype(jnp.bfloat16))
        total = total + part.astype(jnp.float32)
    return total

def reference(layer_input_tokens, attention_norm_gain, query_projection, key_projection, value_projection, decay_first_factor, decay_second_factor, decay_logit_bias, extra_log_decay, head_output_gain, attention_output_projection, feedforward_norm_gain, gate_projection, up_projection, down_projection):
    normed = norm_rows(layer_input_tokens, attention_norm_gain).astype(jnp.bfloat16)
    query = jnp.dot(normed, query_projection, preferred_element_type=jnp.float32).astype(jnp.bfloat16)
    key = jnp.dot(normed, key_projection, preferred_element_type=jnp.float32).astype(jnp.bfloat16)
    value = jnp.dot(normed, value_projection, preferred_element_type=jnp.float32).astype(jnp.bfloat16)
    lowrank = jnp.dot(normed, decay_first_factor, preferred_element_type=jnp.float32).astype(jnp.bfloat16)
    decay_logit_values = jnp.dot(lowrank, decay_second_factor, preferred_element_type=jnp.float32) + decay_logit_bias
    decay_logarithm = jax.nn.log_sigmoid(decay_logit_values) / normed_gate + jnp.repeat(extra_log_decay, KEY_CHANNELS, axis=1)

    def sequences(array, width):
        return array.astype(jnp.float32).reshape(N_FS, SEQ_LEN, HEADS, width)
    mixed = jax.vmap(jax.vmap(both_ways, in_axes=1, out_axes=1))(sequences(query, KEY_CHANNELS), sequences(key, KEY_CHANNELS), sequences(value, DV), sequences(decay_logarithm, KEY_CHANNELS))
    headed = head_norm(mixed.reshape(TOKENS, HEADS, DV), head_output_gain)
    headed = headed.reshape(TOKENS, HEADS * DV).astype(jnp.bfloat16)
    mixer = group_sum(headed, attention_output_projection)
    residual = (layer_input_tokens.astype(jnp.float32) + mixer).astype(jnp.bfloat16)
    second = norm_rows(residual, feedforward_norm_gain).astype(jnp.bfloat16)
    gate = jnp.dot(second, gate_projection, preferred_element_type=jnp.float32)
    up = jnp.dot(second, up_projection, preferred_element_type=jnp.float32)
    hidden = (jax.nn.silu(gate) * up).astype(jnp.bfloat16)
    channel = group_sum(hidden, down_projection)
    return (residual.astype(jnp.float32) + channel).astype(jnp.bfloat16)
```

```python
import functools

import jax
import jax.numpy as jnp
from jax import lax
from jax.experimental import pallas as pl
from jax.experimental.pallas import tpu as pltpu
from jax.sharding import PartitionSpec as P

MESH = pl.DeviceIdType.MESH
BLOCK = 64
LANES = 128
GATE = 16.0
EPS = 1e-06
CHUNKS = 2
F32 = jnp.float32
BF16 = jnp.bfloat16


def mm(a, b):
    return lax.dot_general(a, b, (((1,), (0,)), ((), ())), preferred_element_type=F32)


def mm_nt(a, b):
    return lax.dot_general(a, b, (((1,), (1,)), ((), ())), preferred_element_type=F32)


def mm_tn(a, b):
    return lax.dot_general(a, b, (((0,), (0,)), ((), ())), preferred_element_type=F32)


def iota(shape, dim):
    return lax.broadcasted_iota(jnp.int32, shape, dim)


def scaled_rows(wide, gain):
    return wide * lax.rsqrt(jnp.mean(wide * wide, axis=-1, keepdims=True) + EPS) * gain


def kernel(
    size, paired,
    x_ref, gain1_ref, wq_ref, wk_ref, wv_ref, first_ref, second_ref, bias_ref, extra_ref,
    hgain_ref, wo_ref, gain2_ref, wg_ref, wu_ref, wd_ref,
    out_ref,
    g_qkv, g_out, g_gu, g_dn,
    normed, decs, ends, qs, ks, vs, inside, ups_f, ups_b, car, headed, wout,
    place, hid, wide_gu, part_own, part_send, part_recv, ring_tx, ring_rx, own_res, full2, full3,
    z_send, z_recv, y_send, y_recv, rs_send, rs_recv, ag_send, ag_recv, out_sem,
):
    n, tp = size["fs"], size["tp"]
    chips = tp // 2
    far = chips // 2
    grp, me, t = lax.axis_index("grp"), lax.axis_index("fs"), lax.axis_index("tp")
    chip, core = t // 2, t % 2
    half = grp % 2 if paired else 0
    up_z, down_z = lax.rem(me + 1, n), lax.rem(me + n - 1, n)
    twin = grp + 1 - 2 * (grp % 2)
    mate = t + 1 - 2 * core
    right, left = lax.rem(t + 2, tp), lax.rem(t + tp - 2, tp)
    rows = x_ref.shape[0]
    share = rows // tp
    blocks = rows // BLOCK
    keyw = wq_ref.shape[1]
    valw = wv_ref.shape[1]
    wide = x_ref.shape[1]
    cols = wide // CHUNKS
    ffw = wg_ref.shape[1]
    whole = ffw // LANES * LANES
    rest = ffw - whole

    g_qkv[me, :, 0:keyw] = wq_ref[...]
    g_qkv[me, :, keyw : 2 * keyw] = wk_ref[...]
    g_qkv[me, :, 2 * keyw :] = wv_ref[...]
    g_out[me] = wo_ref[...]
    g_gu[me, :, 0:whole] = wg_ref[:, 0:whole]
    g_gu[me, :, whole : 2 * whole] = wu_ref[:, 0:whole]
    g_gu[me, :, 2 * whole :] = jnp.concatenate([wg_ref[:, whole:], wu_ref[:, whole:]], axis=1)
    dn_rows = wd_ref.shape[0]
    for c in range(CHUNKS):
        g_dn[c, me] = jnp.zeros(g_dn.shape[2:], BF16)
        g_dn[c, me, 0:dn_rows, :] = wd_ref[:, c * cols : (c + 1) * cols]

    barrier = pltpu.get_barrier_semaphore()
    friends = [{"fs": up_z}, {"fs": down_z}, {"tp": mate}, {"tp": right}, {"tp": left}]
    if paired:
        friends.append({"grp": twin})
    for friend in friends:
        pl.semaphore_signal(barrier, inc=1, device_id=friend, device_id_type=MESH)
    pl.semaphore_wait(barrier, len(friends))

    depth = wq_ref.shape[0]
    strip = depth // 2 if paired else depth
    gu_strip = strip // 2

    def part_of(ref, count, offset):
        base = half * (depth // 2) + offset
        return lambda slot: ref.at[slot, pl.ds(pl.multiple_of(base, 16), count), :]

    QKV, OUT, GUA, GUB, DNL, DNR = range(6)
    views = [
        part_of(g_qkv, strip, 0),
        lambda slot: g_out.at[slot],
        part_of(g_gu, gu_strip, 0),
        part_of(g_gu, gu_strip, gu_strip),
        lambda slot: g_dn.at[0, slot],
        lambda slot: g_dn.at[1, slot],
    ]
    crossing = {QKV: 0, GUA: 1, GUB: 2} if paired else {}
    hops = (n // 2, n - 1 - n // 2)

    def z_copy(p, way, s):
        slot = lax.rem(me - s + n, n) if way == 0 else lax.rem(me + s, n)
        view = views[p](slot)
        return pltpu.make_async_remote_copy(
            src_ref=view, dst_ref=view,
            send_sem=z_send.at[p, way, s], recv_sem=z_recv.at[p, way, s],
            device_id={"fs": up_z if way == 0 else down_z}, device_id_type=MESH,
        )

    def y_copy(p, way, s):
        slot = lax.rem(me - s - 1 + n, n) if way == 0 else lax.rem(me + s + 1, n)
        view = views[p](slot)
        return pltpu.make_async_remote_copy(
            src_ref=view, dst_ref=view,
            send_sem=y_send.at[crossing[p], way, s], recv_sem=y_recv.at[crossing[p], way, s],
            device_id={"grp": twin}, device_id_type=MESH,
        )

    def step(p, s, ways=(0, 1), arrive=True, leave=True):
        for way in ways:
            if arrive:
                z_copy(p, way, s - 1).wait_recv()
            if leave:
                z_copy(p, way, s).start()
            if arrive and p in crossing:
                y_copy(p, way, s - 1).start()

    def at(p, s):
        for way in (0, 1):
            if s <= hops[way]:
                step(p, s, (way,), arrive=s > 0, leave=s < hops[way])

    def y_arrived(p):
        if p in crossing:
            for way in (0, 1):

                @pl.loop(0, hops[way])
                def _(s):
                    y_copy(p, way, s).wait_recv()

    late = n // 4
    starts = {QKV: 0, OUT: 0, GUA: 0, GUB: late, DNL: n // 2, DNR: n // 2 + 2}
    queue = []

    def fill(lo, hi):
        for tick in range(lo, hi):
            queue.append([(p, tick - b) for p, b in starts.items() if 0 <= tick - b <= n // 2])

    def pump(count=1):
        for _ in range(count):
            if queue:
                for p, s in queue.pop(0):
                    at(p, s)

    low = iota((BLOCK, BLOCK), 0) >= iota((BLOCK, BLOCK), 1)
    high = iota((BLOCK, BLOCK), 0) <= iota((BLOCK, BLOCK), 1)

    def prepare(b):
        span = pl.ds(pl.multiple_of(b * BLOCK, BLOCK), BLOCK)
        tidy = scaled_rows(x_ref[span, :].astype(F32), gain1_ref[...]).astype(BF16)
        normed[span, :] = tidy
        lowrank = mm(tidy, first_ref[...]).astype(BF16)
        logits = mm(lowrank, second_ref[...]) + bias_ref[...]
        logsig = jnp.minimum(logits, 0.0) - jnp.log1p(jnp.exp(-jnp.abs(logits)))
        dec = logsig / GATE + extra_ref[span, :]
        one = dec.astype(BF16)
        left_over = dec - one.astype(F32)
        two = left_over.astype(BF16)
        three = (left_over - two.astype(F32)).astype(BF16)
        terms = jnp.concatenate([one, two, three], axis=1)
        for way, mask in ((0, low), (1, high)):
            sums = mm(jnp.where(mask, 1.0, 0.0).astype(BF16), terms)
            run = sums[:, 0:keyw] + sums[:, keyw : 2 * keyw] + sums[:, 2 * keyw :]
            mid_row = BLOCK // 2 - 1 if way == 0 else BLOCK // 2
            end_row = BLOCK - 1 if way == 0 else 0
            middle = run[mid_row : mid_row + 1, :]
            closing = run[end_row : end_row + 1, :]
            decs[way, 0, span, :] = jnp.exp(run)
            decs[way, 1, span, :] = jnp.exp(run - middle)
            decs[way, 2, span, :] = jnp.exp(middle - run)
            decs[way, 3, span, :] = jnp.exp(closing - run)
            ends[way, b] = jnp.broadcast_to(jnp.exp(closing), (8, keyw))

    for p in (QKV, OUT, GUA):
        at(p, 0)

    def early(lo, hi, pieces, with_rows):
        def body(tick, carry):
            for p in pieces:
                step(p, tick - starts[p])
            if with_rows:
                prepare(tick - 1)
            return carry

        lax.fori_loop(lo, hi, body, 0)

    ready = min(late - 1, blocks)
    if late > 1:
        early(1, 1 + ready, (QKV, OUT, GUA), True)
        if 1 + ready < late:
            early(1 + ready, late, (QKV, OUT, GUA), False)

    def rest_rows(b, carry):
        prepare(b)
        return carry

    at(QKV, late), at(OUT, late), at(GUA, late), at(GUB, 0)
    lax.fori_loop(ready, blocks, rest_rows, 0)
    last = max(n // 2 - 1, late + 1)
    if late + 1 < last:
        early(late + 1, last, (QKV, OUT, GUA, GUB), False)
    place_rows = iota(place.shape, 0)
    place_cols = iota(place.shape, 1)
    padded = g_dn.shape[2]
    place[...] = jnp.where(
        (place_rows // dn_rows == place_cols // padded)
        & (place_rows % dn_rows == place_cols % padded),
        1.0,
        0.0,
    ).astype(BF16)
    fill(last, n + 3)
    pump(2)
    y_arrived(QKV)

    def project(lo, hi):
        return mm(normed[...], g_qkv[:, :, lo:hi].reshape(n * depth, hi - lo)).astype(BF16)

    both = project(0, 2 * keyw)
    qs[...] = both[:, 0:keyw]
    ks[...] = both[:, keyw:]
    pump()
    vs[...] = project(2 * keyw, 2 * keyw + valw)
    pump()

    for b in range(blocks):
        span = slice(b * BLOCK, (b + 1) * BLOCK)
        q, k, v = qs[span, :].astype(F32), ks[span, :].astype(F32), vs[span, :]
        scores = 0.0
        for way, mask in ((0, low), (1, high)):
            pair = mm_nt(
                (q * decs[way, 1, span, :]).astype(BF16), (k * decs[way, 2, span, :]).astype(BF16)
            )
            scores = scores + jnp.where(mask, pair, 0.0)
            (ups_f, ups_b)[way][b] = mm_tn(v, (k * decs[way, 3, span, :]).astype(BF16))
        inside[span, :] = mm(scores.astype(BF16), v)
        if b % 2 == 1:
            pump()
    for way, ups, order in ((0, ups_f, range(blocks)), (1, ups_b, range(blocks - 1, -1, -1))):
        state = jnp.zeros((valw, keyw), F32)
        for b in order:
            car[b, :, way * keyw : (way + 1) * keyw] = state.astype(BF16)
            state = state * ends[way, b, 0:1, :] + ups[b]
    pump()
    wout[...] = g_out[...].astype(F32).reshape(wout.shape).astype(BF16)
    for b in range(blocks):
        span = slice(b * BLOCK, (b + 1) * BLOCK)
        q = qs[span, :].astype(F32)
        reach = jnp.concatenate(
            [(q * decs[0, 0, span, :]).astype(BF16), (q * decs[1, 0, span, :]).astype(BF16)], axis=1
        )
        mixed = inside[span, :] + mm_nt(reach, car[b])
        headed[b] = scaled_rows(mixed, hgain_ref[...]).astype(BF16)
        if b % 4 == 3:
            pump()

    low_rows, high_rows = slice(0, share // 2), slice(share // 2, share)

    def chip_rows(ref, which):
        return jnp.concatenate([ref[2 * i + which] for i in range(chips)], axis=0)

    def rs_copy(q, k, src, dst, to):
        return pltpu.make_async_remote_copy(
            src_ref=src, dst_ref=dst, send_sem=rs_send.at[q, k], recv_sem=rs_recv.at[q, k],
            device_id={"tp": to}, device_id_type=MESH,
        )

    def ring_copy(q, k):
        return rs_copy(q, 1 + k, ring_tx.at[q, k], ring_rx.at[q, k], right if k < 3 else left)

    def pair_copy(q):
        return rs_copy(q, 0, part_send.at[q], part_recv.at[q], mate)

    def rs_multiply(q, source, weight):
        other = mm(chip_rows(source, 1 - core), weight)
        part_send[q] = other.astype(BF16).reshape(part_send.shape[1:])
        pair_copy(q).start()
        part_own[q] = mm(chip_rows(source, core), weight).reshape(part_own.shape[1:])

    ahead, behind = lax.rem(chip + 1, chips), lax.rem(chip + chips - 1, chips)
    across = lax.rem(chip + far, chips)

    def chip_sum(q, which, span):
        return part_own[q, which, span, :] + part_recv[q, which, span, :].astype(F32)

    def rs_send_off(q):
        pair_copy(q).wait_recv()
        ring_tx[q, 0] = chip_sum(q, across, low_rows).astype(BF16)
        ring_tx[q, 3] = chip_sum(q, across, high_rows).astype(BF16)
        ring_copy(q, 0).start()
        ring_copy(q, 3).start()
        ring_tx[q, 1] = chip_sum(q, ahead, high_rows).astype(BF16)
        ring_tx[q, 4] = chip_sum(q, behind, low_rows).astype(BF16)
        ring_copy(q, 1).start()
        ring_copy(q, 4).start()

    def rs_relay(q):
        ring_copy(q, 0).wait_recv()
        ring_tx[q, 2] = (chip_sum(q, ahead, low_rows) + ring_rx[q, 0].astype(F32)).astype(BF16)
        ring_copy(q, 2).start()
        ring_copy(q, 3).wait_recv()
        ring_tx[q, 5] = (chip_sum(q, behind, high_rows) + ring_rx[q, 3].astype(F32)).astype(BF16)
        ring_copy(q, 5).start()

    def rs_finish(q):
        for k in (1, 2, 4, 5):
            ring_copy(q, k).wait_recv()
        top = chip_sum(q, chip, low_rows) + ring_rx[q, 2].astype(F32) + ring_rx[q, 4].astype(F32)
        end = chip_sum(q, chip, high_rows) + ring_rx[q, 1].astype(F32) + ring_rx[q, 5].astype(F32)
        return jnp.concatenate([top, end], axis=0)

    def ag_copy(a, k, buf):
        opposite = lax.rem(t + 2 * far, tp)
        slot, span, to = [
            (t, None, mate),
            (t, None, right),
            (t, None, left),
            (left, low_rows, right),
            (right, high_rows, left),
            (left, None, mate),
            (right, None, mate),
            (opposite, low_rows, mate),
            (opposite, high_rows, mate),
        ][k]
        view = buf.at[slot] if span is None else buf.at[slot, span, :]
        return pltpu.make_async_remote_copy(
            src_ref=view, dst_ref=view, send_sem=ag_send.at[a, k], recv_sem=ag_recv.at[a, k],
            device_id={"tp": to}, device_id_type=MESH,
        )

    def ag_start(a, buf):
        for k in (1, 2, 0):
            ag_copy(a, k, buf).start()

    def ag_relay(a, buf):
        ag_copy(a, 1, buf).wait_recv()
        ag_copy(a, 3, buf).start()
        ag_copy(a, 5, buf).start()
        ag_copy(a, 2, buf).wait_recv()
        ag_copy(a, 4, buf).start()
        ag_copy(a, 6, buf).start()

    def ag_finish(a, buf):
        ag_copy(a, 3, buf).wait_recv()
        ag_copy(a, 7, buf).start()
        ag_copy(a, 4, buf).wait_recv()
        ag_copy(a, 8, buf).start()
        for k in (0, 5, 6, 7, 8):
            ag_copy(a, k, buf).wait_recv()

    for c in range(CHUNKS):
        rs_multiply(c, headed, wout[:, c * cols : (c + 1) * cols])
        pump()
    for c in range(CHUNKS):
        rs_send_off(c)
        pump()
    for c in range(CHUNKS):
        rs_relay(c)
        pump()
    own_rows = pl.ds(pl.multiple_of(t * share, share), share)
    for c in range(CHUNKS):
        span = slice(c * cols, (c + 1) * cols)
        own_res[:, span] = (x_ref[own_rows, span].astype(F32) + rs_finish(c)).astype(BF16)
    full2[t] = scaled_rows(own_res[...].astype(F32), gain2_ref[...]).astype(BF16)
    ag_start(0, full2)
    pump(2)
    ag_relay(0, full2)
    pump(2)
    ag_finish(0, full2)
    while sum(len(q) for q in queue if any(p == GUB for p, _ in q)):
        pump()
    y_arrived(GUA)
    y_arrived(GUB)

    normed2 = full2[...].reshape(rows, wide)
    for lo in range(0, 2 * ffw, 2 * LANES):
        hi = min(lo + 2 * LANES, 2 * ffw)
        wide_gu[:, lo:hi] = mm(normed2, g_gu[:, :, lo:hi].reshape(n * depth, hi - lo))
    for i in range(tp):
        span = slice(i * share, (i + 1) * share)
        tail = wide_gu[span, 2 * whole :]
        gate = jnp.concatenate([wide_gu[span, 0:whole], tail[:, 0:rest]], axis=1)
        up = jnp.concatenate([wide_gu[span, whole : 2 * whole], tail[:, rest:]], axis=1)
        hidden = (gate / (1.0 + jnp.exp(-gate)) * up).astype(BF16)
        hid[i] = mm(hidden, place[...]).astype(BF16)
    pump()

    for c in range(CHUNKS):
        while sum(len(q) for q in queue if any(p == DNL + c for p, _ in q)):
            pump()
        q = CHUNKS + c
        weight = g_dn[c].astype(F32).reshape(n * padded, cols).astype(BF16)
        rs_multiply(q, hid, weight)
        if c > 0:
            rs_relay(q - 1)
        rs_send_off(q)

    def finish(c):
        span = slice(c * cols, (c + 1) * cols)
        done = own_res[:, span].astype(F32) + rs_finish(CHUNKS + c)
        full3[c, t] = done.astype(BF16)
        ag_start(1 + c, full3.at[c])

    def put(c):
        return pltpu.make_async_copy(
            full3.at[c], out_ref.at[:, :, c * cols : (c + 1) * cols], out_sem.at[c]
        )

    finish(0)
    rs_relay(CHUNKS + 1)
    ag_relay(1, full3.at[0])
    finish(1)
    ag_finish(1, full3.at[0])
    put(0).start()
    ag_relay(2, full3.at[1])
    ag_finish(2, full3.at[1])
    put(1).start()

    for p in range(len(views)):
        for way in (0, 1):

            @pl.loop(0, hops[way])
            def _(s):
                z_copy(p, way, s).wait_send()
                if p in crossing:
                    y_copy(p, way, s).wait_send()

    for q in range(2 * CHUNKS):
        pair_copy(q).wait_send()
        for k in range(6):
            ring_copy(q, k).wait_send()
    for a, buf in ((0, full2), (1, full3.at[0]), (2, full3.at[1])):
        for k in range(9):
            ag_copy(a, k, buf).wait_send()
    for c in range(CHUNKS):
        put(c).wait()


def shards(size, *args):
    (x, gain1, wq, wk, wv, first, second, bias, extra, hgain, wo, gain2, wg, wu, wd) = args
    n, tp = size["fs"], size["tp"]
    paired = size["grp"] % 2 == 0
    rows, wide = x.shape
    depth, keyw = wq.shape
    valw, ffw = wv.shape[1], wg.shape[1]
    share, chips, blocks = rows // tp, tp // 2, rows // BLOCK
    cols = wide // CHUNKS
    padded = -(-wd.shape[0] // 8) * 8
    sems = pltpu.SemaphoreType.DMA
    vmem = pltpu.VMEM
    steps = n // 2
    out = pl.pallas_call(
        functools.partial(kernel, size, paired),
        out_shape=jax.ShapeDtypeStruct((tp, share, wide), BF16),
        in_specs=[pl.BlockSpec(memory_space=pltpu.VMEM)] * 15,
        out_specs=pl.BlockSpec(memory_space=pl.ANY),
        scratch_shapes=[
            vmem((n, depth, 2 * keyw + valw), BF16),
            vmem((n, wo.shape[0], wide), BF16),
            vmem((n, depth, 2 * ffw), BF16),
            vmem((CHUNKS, n, padded, cols), BF16),
            vmem((rows, wide), BF16),
            vmem((2, 4, rows, keyw), F32),
            vmem((2, blocks, 8, keyw), F32),
            vmem((rows, keyw), BF16),
            vmem((rows, keyw), BF16),
            vmem((rows, valw), BF16),
            vmem((rows, valw), F32),
            vmem((blocks, valw, keyw), F32),
            vmem((blocks, valw, keyw), F32),
            vmem((blocks, valw, 2 * keyw), BF16),
            vmem((blocks, BLOCK, valw), BF16),
            vmem((n * wo.shape[0], wide), BF16),
            vmem((ffw, n * padded), BF16),
            vmem((tp, share, n * padded), BF16),
            vmem((rows, 2 * ffw), F32),
            vmem((2 * CHUNKS, chips, share, cols), F32),
            vmem((2 * CHUNKS, chips, share, cols), BF16),
            vmem((2 * CHUNKS, chips, share, cols), BF16),
            vmem((2 * CHUNKS, 6, share // 2, cols), BF16),
            vmem((2 * CHUNKS, 6, share // 2, cols), BF16),
            vmem((share, wide), BF16),
            vmem((tp, share, wide), BF16),
            vmem((CHUNKS, tp, share, cols), BF16),
            sems((6, 2, steps)),
            sems((6, 2, steps)),
            sems((3, 2, steps)),
            sems((3, 2, steps)),
            sems((2 * CHUNKS, 7)),
            sems((2 * CHUNKS, 7)),
            sems((1 + CHUNKS, 9)),
            sems((1 + CHUNKS, 9)),
            sems((CHUNKS,)),
        ],
        compiler_params=pltpu.CompilerParams(
            collective_id=0, has_side_effects=True, vmem_limit_bytes=64 * 1024 * 1000
        ),
        name="layer",
    )(
        x, gain1.reshape(1, -1), wq, wk, wv, first, second, bias.reshape(1, -1), extra,
        hgain.reshape(1, -1), wo, gain2.reshape(1, -1), wg, wu, wd,
    )
    return out.reshape(rows, wide)


def solution(mesh):
    placed = (
        P(("grp", "fs"), None),
        P(),
        P("fs", "tp"),
        P("fs", "tp"),
        P("fs", "tp"),
        P(),
        P(None, "tp"),
        P("tp"),
        P(("grp", "fs"), "tp"),
        P(),
        P(("tp", "fs"), None),
        P(),
        P("fs", "tp"),
        P("fs", "tp"),
        P(("tp", "fs"), None),
    )
    return jax.shard_map(
        functools.partial(shards, dict(mesh.shape)),
        mesh=mesh, in_specs=placed, out_specs=P(("grp", "fs"), None), check_vma=False,
    )
```

```python
import functools

import jax
import jax.numpy as jnp
from jax import lax
from jax.experimental import pallas as pl
from jax.experimental.pallas import tpu as pltpu
from jax.sharding import PartitionSpec as P

MESH = pl.DeviceIdType.MESH
BLOCK = 64
LANES = 128
GATE = 16.0
EPS = 1e-06
MIX_CHUNKS = 2
FF_CHUNKS = 2
VMEM_MIB = 60
GU_ROWS = (16, 16)
DN_SPLIT = (1, 1)
START = {"qkv": 0, "out": 0, "gu0": 7, "gu1": 8, "dn0": 9, "dn1": 11}
PUMP = (1, 1, 1, 1, 2, 1, 1, 1, 1)
F32 = jnp.float32
BF16 = jnp.bfloat16


def mm(a, b):
    return lax.dot_general(a, b, (((1,), (0,)), ((), ())), preferred_element_type=F32)


def mm_nt(a, b):
    return lax.dot_general(a, b, (((1,), (1,)), ((), ())), preferred_element_type=F32)


def mm_tn(a, b):
    return lax.dot_general(a, b, (((0,), (0,)), ((), ())), preferred_element_type=F32)


def iota(shape, dim):
    return lax.broadcasted_iota(jnp.int32, shape, dim)


def scaled_rows(wide, gain):
    return wide * lax.rsqrt(jnp.mean(wide * wide, axis=-1, keepdims=True) + EPS) * gain


def kernel(
    size, paired, arrived,
    x_ref, gain1_ref, wq_ref, wk_ref, wv_ref, first_ref, second_ref, bias_ref, extra_ref,
    hgain_ref, wo_ref, gain2_ref, wg_ref, wu_ref, wd_ref,
    out_ref,
    g_qkv, g_out, g_gu, g_dn,
    normed, extra_col, decs, ends, qs, ks, vs, inside, ups_f, ups_b, car, headed, wout,
    place, hid, wide_gu, mix_bufs, ff_bufs, own_res, full2, full3,
    z_send, z_recv, y_send, y_recv, ag_send, ag_recv, out_sem,
):
    n, tp = size["fs"], size["tp"]
    chips = tp // 2
    far = chips // 2
    grp, me, t = lax.axis_index("grp"), lax.axis_index("fs"), lax.axis_index("tp")
    chip, core = t // 2, t % 2
    half = grp % 2 if paired else 0
    up_z, down_z = lax.rem(me + 1, n), lax.rem(me + n - 1, n)
    twin = grp + 1 - 2 * (grp % 2)
    mate = t + 1 - 2 * core
    right, left = lax.rem(t + 2, tp), lax.rem(t + tp - 2, tp)
    rows = x_ref.shape[0]
    share = rows // tp
    blocks = rows // BLOCK
    keyw = wq_ref.shape[1]
    valw = wv_ref.shape[1]
    wide = x_ref.shape[1]
    mix_cols, cols = wide // MIX_CHUNKS, wide // FF_CHUNKS
    ffw = wg_ref.shape[1]
    whole = ffw // LANES * LANES
    rest = ffw - whole

    barrier = pltpu.get_barrier_semaphore()
    up_two, down_two = lax.rem(me + 2, n), lax.rem(me + n - 2, n)
    friends = [{"fs": z} for z in (up_z, down_z, up_two, down_two)]
    friends += [{"tp": mate}, {"tp": right}, {"tp": left}]
    if paired:
        friends.append({"grp": twin})
    for friend in friends:
        pl.semaphore_signal(barrier, inc=1, device_id=friend, device_id_type=MESH)

    arrived(range(1, 15))
    g_qkv[me, :, 0:keyw] = wq_ref[...]
    g_qkv[me, :, keyw : 2 * keyw] = wk_ref[...]
    g_qkv[me, :, 2 * keyw :] = wv_ref[...]
    g_out[me] = wo_ref[...]
    g_gu[me, :, 0:whole] = wg_ref[:, 0:whole]
    g_gu[me, :, whole : 2 * whole] = wu_ref[:, 0:whole]
    g_gu[me, :, 2 * whole :] = jnp.concatenate([wg_ref[:, whole:], wu_ref[:, whole:]], axis=1)
    dn_rows = wd_ref.shape[0]
    for c in range(FF_CHUNKS):
        g_dn[c, me] = jnp.zeros(g_dn.shape[2:], BF16)
        g_dn[c, me, 0:dn_rows, :] = wd_ref[:, c * cols : (c + 1) * cols]
    eye = iota((BLOCK, BLOCK), 0) == iota((BLOCK, BLOCK), 1)
    for b in range(blocks):
        span = slice(b * BLOCK, (b + 1) * BLOCK)
        extra_col[span, :] = jnp.sum(jnp.where(eye, extra_ref[:, span], 0.0), axis=1, keepdims=True)
    pl.semaphore_wait(barrier, len(friends))

    depth = wq_ref.shape[0]
    lot = depth // 2 if paired else depth

    def part_of(ref, first, count):
        return lambda slots: ref.at[slots, pl.ds(pl.multiple_of(half * lot + first, 8), count), :]

    QKV, OUT = "qkv", "out"
    out_cols = wide // 2 if paired else wide

    def out_part(slots):
        return g_out.at[slots, :, pl.ds(pl.multiple_of(half * out_cols, LANES), out_cols)]

    views = {QKV: part_of(g_qkv, 0, lot), OUT: out_part}
    strided = (QKV, OUT)
    GU, DN = [], []
    first = 0
    for k, count in enumerate(GU_ROWS):
        count = count * lot // sum(GU_ROWS)
        GU.append(f"gu{k}")
        views[GU[k]] = part_of(g_gu, first, count)
        first += count
    first = 0
    for k, count in enumerate(DN_SPLIT):
        views[f"dn{k}"] = lambda slots, first=first, count=count: g_dn.at[pl.ds(first, count), slots]
        DN += [f"dn{k}"] * count
        first += count
    number = {p: i for i, p in enumerate(views)}
    crossing = {p: i for i, p in enumerate([QKV, OUT] + GU)} if paired else {}
    hops = (n // 2, n - 1 - n // 2)

    def z_copy(p, way, s, view=None):
        if view is None:
            view = views[p](lax.rem(me - s + n, n) if way == 0 else lax.rem(me + s, n))
        return pltpu.make_async_remote_copy(
            src_ref=view, dst_ref=view,
            send_sem=z_send.at[number[p], way], recv_sem=z_recv.at[number[p], way, s],
            device_id={"fs": up_z if way == 0 else down_z}, device_id_type=MESH,
        )

    def y_copy(p, view):
        return pltpu.make_async_remote_copy(
            src_ref=view, dst_ref=view,
            send_sem=y_send.at[crossing[p]], recv_sem=y_recv.at[crossing[p]],
            device_id={"grp": twin}, device_id_type=MESH,
        )

    def cross(p, way, s):
        slot = lax.rem(me - s - 1 + n, n) if way == 0 else lax.rem(me + s + 1, n)
        y_copy(p, views[p](slot)).start()

    def step(p, s, ways=(0, 1), arrive=True, leave=True):
        for way in ways:
            if arrive:
                z_copy(p, way, s - 1).wait_recv()
            if leave:
                z_copy(p, way, s).start()
            if arrive and p in crossing:
                cross(p, way, s - 1)

    def away(way, distance):
        return lax.rem(me - distance + n, n) if way == 0 else lax.rem(me + distance, n)

    def far_copy(p, way, distance, two):
        view = views[p](away(way, distance))
        to = (up_two if two else up_z) if way == 0 else (down_two if two else down_z)
        return pltpu.make_async_remote_copy(
            src_ref=view, dst_ref=view, send_sem=z_send.at[number[p], way],
            recv_sem=z_recv.at[number[p], way, distance + (1 if two else 0)],
            device_id={"fs": to}, device_id_type=MESH,
        )

    def far_step(p, j):
        known = isinstance(j, int)
        for way in (0, 1):
            for distance in (2 * j - 1, 2 * j):
                if not known or distance <= hops[way]:
                    z_copy(p, way, distance - 1).wait_recv()
                    if not known or distance <= hops[way] - 2:
                        far_copy(p, way, distance, True).start()
                    if p in crossing:
                        cross(p, way, distance - 1)

    def at(p, s):
        if p in strided:
            if s > 0:
                far_step(p, s)
            else:
                for way in (0, 1):
                    far_copy(p, way, 0, False).start()
                    far_copy(p, way, 0, True).start()
            return
        for way in (0, 1):
            if s <= hops[way]:
                step(p, s, (way,), arrive=s > 0, leave=s < hops[way])

    def y_arrived(p):
        if p in crossing:
            y_copy(p, views[p](pl.ds(0, n - 1))).wait_recv()

    starts = {p: START[p] for p in views}
    order = sorted(views, key=lambda p: (starts[p], number[p]))
    clock = [0]
    final = {p: n // 4 if p in strided else n // 2 for p in views}
    even = {p: n // 4 - 1 if p in strided else hops[1] for p in views}

    def pump(count=1):
        for _ in range(count):
            tick = clock[0]
            for p in order:
                if 0 <= tick - starts[p] <= final[p]:
                    at(p, tick - starts[p])
            clock[0] += 1

    def complete(p):
        while clock[0] <= starts[p] + final[p]:
            pump()

    def glide(count, beside):
        end = clock[0] + count
        while clock[0] < end:
            tick = clock[0]
            inner = [p for p in order if 1 <= tick - starts[p] < even[p]]
            length = 0
            while tick + length < end and all(
                (1 <= tick + length - starts[p] < even[p])
                if p in inner
                else not 0 <= tick + length - starts[p] <= final[p]
                for p in order
            ):
                length += 1
            if length < 3:
                pump()
                beside(tick)
                continue

            def body(now, carry, inner=inner):
                for p in inner:
                    (far_step if p in strided else step)(p, now - starts[p])
                beside(now)
                return carry

            lax.fori_loop(tick, tick + length, body, 0)
            clock[0] += length

    def drain(p):
        for way in (0, 1):
            z_copy(p, way, 0, views[p](pl.ds(0, hops[way]))).wait_send()
        if p in crossing:
            y_copy(p, views[p](pl.ds(0, n - 1))).wait_send()

    low = iota((BLOCK, BLOCK), 0) >= iota((BLOCK, BLOCK), 1)
    high = iota((BLOCK, BLOCK), 0) <= iota((BLOCK, BLOCK), 1)

    def prepare(b):
        span = pl.ds(pl.multiple_of(b * BLOCK, BLOCK), BLOCK)
        tidy = scaled_rows(x_ref[span, :].astype(F32), gain1_ref[...]).astype(BF16)
        normed[span, :] = tidy
        lowrank = mm_nt(tidy, first_ref[...]).astype(BF16)
        logits = mm(lowrank, second_ref[...]) + bias_ref[...]
        logsig = jnp.minimum(logits, 0.0) - jnp.log1p(jnp.exp(-jnp.abs(logits)))
        dec = logsig / GATE + extra_col[span, :]
        one = dec.astype(BF16)
        left_over = dec - one.astype(F32)
        two = left_over.astype(BF16)
        three = (left_over - two.astype(F32)).astype(BF16)
        terms = jnp.concatenate([one, two, three], axis=1)
        for way, mask in ((0, low), (1, high)):
            sums = mm(jnp.where(mask, 1.0, 0.0).astype(BF16), terms)
            run = sums[:, 0:keyw] + sums[:, keyw : 2 * keyw] + sums[:, 2 * keyw :]
            mid_row = BLOCK // 2 - 1 if way == 0 else BLOCK // 2
            end_row = BLOCK - 1 if way == 0 else 0
            middle = run[mid_row : mid_row + 1, :]
            closing = run[end_row : end_row + 1, :]
            decs[way, 0, span, :] = jnp.exp(run)
            decs[way, 1, span, :] = jnp.exp(run - middle)
            decs[way, 2, span, :] = jnp.exp(middle - run)
            decs[way, 3, span, :] = jnp.exp(closing - run)
            ends[way, b] = jnp.broadcast_to(jnp.exp(closing), (8, keyw))

    pump()
    arrived([0])

    glide(min(blocks, n // 2 - 1), lambda tick: prepare(tick - 1))
    for b in range(min(blocks, n // 2 - 1), blocks):
        prepare(b)
    place_rows = iota(place.shape, 0)
    place_cols = iota(place.shape, 1)
    padded = g_dn.shape[2]
    place[...] = jnp.where(
        (place_rows // dn_rows == place_cols // padded)
        & (place_rows % dn_rows == place_cols % padded),
        1.0,
        0.0,
    ).astype(BF16)
    glide(starts[QKV] + final[QKV] + 1 - clock[0], lambda tick: None)
    y_arrived(QKV)

    def project(lo, hi):
        return mm(normed[...], g_qkv[:, :, lo:hi].reshape(n * depth, hi - lo)).astype(BF16)

    both = project(0, 2 * keyw)
    qs[...] = both[:, 0:keyw]
    ks[...] = both[:, keyw:]
    pump(PUMP[0])
    vs[...] = project(2 * keyw, 2 * keyw + valw)

    for b in range(blocks):
        span = slice(b * BLOCK, (b + 1) * BLOCK)
        q, k, v = qs[span, :].astype(F32), ks[span, :].astype(F32), vs[span, :]
        scores = 0.0
        for way, mask in ((0, low), (1, high)):
            pair = mm_nt(
                (q * decs[way, 1, span, :]).astype(BF16), (k * decs[way, 2, span, :]).astype(BF16)
            )
            scores = scores + jnp.where(mask, pair, 0.0)
            (ups_f, ups_b)[way][b] = mm_tn(v, (k * decs[way, 3, span, :]).astype(BF16))
        inside[span, :] = mm(scores.astype(BF16), v)
        if b % 4 == 3:
            pump(PUMP[1])
    for way, ups, blocks_in_turn in ((0, ups_f, range(blocks)), (1, ups_b, range(blocks - 1, -1, -1))):
        state = jnp.zeros((valw, keyw), F32)
        for b in blocks_in_turn:
            car[b, :, way * keyw : (way + 1) * keyw] = state.astype(BF16)
            state = state * ends[way, b, 0:1, :] + ups[b]
    complete(OUT)
    y_arrived(OUT)
    wout[...] = g_out[...].astype(F32).reshape(wout.shape).astype(BF16)
    for b in range(blocks):
        span = slice(b * BLOCK, (b + 1) * BLOCK)
        q = qs[span, :].astype(F32)
        reach = jnp.concatenate(
            [(q * decs[0, 0, span, :]).astype(BF16), (q * decs[1, 0, span, :]).astype(BF16)], axis=1
        )
        mixed = inside[span, :] + mm_nt(reach, car[b])
        headed[b] = scaled_rows(mixed, hgain_ref[...]).astype(BF16)
    pump(PUMP[2])

    low_rows, high_rows = slice(0, share // 2), slice(share // 2, share)

    def chip_rows(ref, which):
        return jnp.concatenate([ref[2 * i + which] for i in range(chips)], axis=0)

    ahead, behind = lax.rem(chip + 1, chips), lax.rem(chip + chips - 1, chips)
    across = lax.rem(chip + far, chips)

    class Sums:
        def __init__(self, bufs):
            self.bufs = bufs
            self.own, self.sent, self.got, self.tx, self.rx = bufs[:5]

        def copy(self, src, dst, sent, got, to):
            return pltpu.make_async_remote_copy(
                src_ref=src, dst_ref=dst, send_sem=sent, recv_sem=got,
                device_id={"tp": to}, device_id_type=MESH,
            )

        def ring(self, q, k):
            return self.copy(
                self.tx.at[q, k], self.rx.at[q, k], self.bufs[5].at[q, 1],
                self.bufs[6].at[q, {0: 1, 3: 2}.get(k, 3)], right if k < 3 else left,
            )

        def rings(self, q, count):
            some = pl.ds(0, count)
            return self.copy(
                self.tx.at[q, some], self.rx.at[q, some], self.bufs[5].at[q, 1],
                self.bufs[6].at[q, 3], right,
            )

        def pair(self, q):
            return self.copy(
                self.sent.at[q], self.got.at[q], self.bufs[5].at[q, 0], self.bufs[6].at[q, 0], mate
            )

        def multiply(self, q, source, weight):
            other = mm(chip_rows(source, 1 - core), weight)
            self.sent[q] = other.astype(BF16).reshape(self.sent.shape[1:])
            self.pair(q).start()
            self.own[q] = mm(chip_rows(source, core), weight).reshape(self.own.shape[1:])

        def of(self, q, which, span):
            return self.own[q, which, span, :] + self.got[q, which, span, :].astype(F32)

        def send_off(self, q):
            self.pair(q).wait_recv()
            self.tx[q, 0] = self.of(q, across, low_rows).astype(BF16)
            self.tx[q, 3] = self.of(q, across, high_rows).astype(BF16)
            self.ring(q, 0).start()
            self.ring(q, 3).start()
            self.tx[q, 1] = self.of(q, ahead, high_rows).astype(BF16)
            self.tx[q, 4] = self.of(q, behind, low_rows).astype(BF16)
            self.ring(q, 1).start()
            self.ring(q, 4).start()

        def relay(self, q):
            self.ring(q, 0).wait_recv()
            self.tx[q, 2] = (self.of(q, ahead, low_rows) + self.rx[q, 0].astype(F32)).astype(BF16)
            self.ring(q, 2).start()
            self.ring(q, 3).wait_recv()
            self.tx[q, 5] = (self.of(q, behind, high_rows) + self.rx[q, 3].astype(F32)).astype(BF16)
            self.ring(q, 5).start()

        def finish(self, q):
            self.rings(q, 4).wait_recv()
            top = self.of(q, chip, low_rows) + self.rx[q, 2].astype(F32) + self.rx[q, 4].astype(F32)
            end = self.of(q, chip, high_rows) + self.rx[q, 1].astype(F32) + self.rx[q, 5].astype(F32)
            return jnp.concatenate([top, end], axis=0)

        def drain(self, q):
            self.pair(q).wait_send()
            self.rings(q, 6).wait_send()

    mix, ff = Sums(mix_bufs), Sums(ff_bufs)

    def ag_copy(a, k, buf):
        opposite = lax.rem(t + 2 * far, tp)
        slot, span, to = [
            (t, None, mate),
            (t, None, right),
            (t, None, left),
            (left, low_rows, right),
            (right, high_rows, left),
            (left, None, mate),
            (right, None, mate),
            (opposite, low_rows, mate),
            (opposite, high_rows, mate),
        ][k]
        view = buf(slot, slice(None) if span is None else span)
        return ag_any(a, view, {1: 0, 2: 1, 3: 2, 4: 3}.get(k, 4), to)

    def ag_any(a, view, got, to):
        return pltpu.make_async_remote_copy(
            src_ref=view, dst_ref=view, send_sem=ag_send.at[a], recv_sem=ag_recv.at[a, got],
            device_id={"tp": to}, device_id_type=MESH,
        )

    def ag_drain(a, buf):
        ag_any(a, buf(pl.ds(0, tp - 1), slice(None)), 0, mate).wait_send()

    def ag_start(a, buf):
        for k in (1, 2, 0):
            ag_copy(a, k, buf).start()

    def ag_relay(a, buf):
        ag_copy(a, 1, buf).wait_recv()
        ag_copy(a, 3, buf).start()
        ag_copy(a, 5, buf).start()
        ag_copy(a, 2, buf).wait_recv()
        ag_copy(a, 4, buf).start()
        ag_copy(a, 6, buf).start()

    def ag_finish(a, buf):
        ag_copy(a, 3, buf).wait_recv()
        ag_copy(a, 7, buf).start()
        ag_copy(a, 4, buf).wait_recv()
        ag_copy(a, 8, buf).start()
        ag_any(a, buf(pl.ds(0, tp // 2), slice(None)), 4, mate).wait_recv()

    def mid_rows(slots, span):
        return full2.at[slots, span, :]

    def last_rows(c):
        return lambda slots, span: full3.at[slots, span, c * cols : (c + 1) * cols]

    for c in range(MIX_CHUNKS):
        mix.multiply(c, headed, wout[:, c * mix_cols : (c + 1) * mix_cols])
    pump(PUMP[3])
    for c in range(MIX_CHUNKS):
        mix.send_off(c)
    pump(PUMP[4])
    mix.relay(0)
    pump(PUMP[5])
    mix.relay(1)
    pump(PUMP[6])
    own_rows = pl.ds(pl.multiple_of(t * share, share), share)
    for c in range(MIX_CHUNKS):
        span = slice(c * mix_cols, (c + 1) * mix_cols)
        own_res[:, span] = (x_ref[own_rows, span].astype(F32) + mix.finish(c)).astype(BF16)
    full2[t] = scaled_rows(own_res[...].astype(F32), gain2_ref[...]).astype(BF16)
    ag_start(0, mid_rows)
    pump(PUMP[7])
    ag_relay(0, mid_rows)
    pump(PUMP[8])
    ag_finish(0, mid_rows)
    for p in GU:
        complete(p)
    for p in GU:
        y_arrived(p)

    normed2 = full2[...].reshape(rows, wide)
    for lo in range(0, 2 * ffw, 2 * LANES):
        hi = min(lo + 2 * LANES, 2 * ffw)
        wide_gu[:, lo:hi] = mm(normed2, g_gu[:, :, lo:hi].reshape(n * depth, hi - lo))
    for i in range(tp):
        span = slice(i * share, (i + 1) * share)
        tail = wide_gu[span, 2 * whole :]
        gate = jnp.concatenate([wide_gu[span, 0:whole], tail[:, 0:rest]], axis=1)
        up = jnp.concatenate([wide_gu[span, whole : 2 * whole], tail[:, rest:]], axis=1)
        hidden = (gate / (1.0 + jnp.exp(-gate)) * up).astype(BF16)
        hid[i] = mm(hidden, place[...]).astype(BF16)
    pump()

    def multiply(c):
        complete(DN[c])
        weight = g_dn[c].astype(F32).reshape(n * padded, cols).astype(BF16)
        ff.multiply(c, hid, weight)

    def finish(c):
        done = own_res[:, c * cols : (c + 1) * cols].astype(F32) + ff.finish(c)
        full3[t, :, c * cols : (c + 1) * cols] = done.astype(BF16)
        ag_start(1 + c, last_rows(c))

    def put(c):
        span = slice(c * cols, (c + 1) * cols)
        return pltpu.make_async_copy(full3.at[:, :, span], out_ref.at[:, :, span], out_sem.at[c])

    def end(c):
        ag_finish(1 + c, last_rows(c))
        put(c).start()

    stages = (multiply, ff.send_off, ff.relay, finish, lambda c: ag_relay(1 + c, last_rows(c)), end)
    idle = [functools.partial(drain, p) for p in order] + [
        functools.partial(mix.drain, c) for c in range(MIX_CHUNKS)
    ] + [functools.partial(ag_drain, 0, mid_rows)]
    for beat in range(FF_CHUNKS + len(stages) - 1):
        for k in reversed(range(len(stages))):
            if 0 <= beat - k < FF_CHUNKS:
                stages[k](beat - k)
        if beat >= FF_CHUNKS:
            for _ in range(3):
                if idle:
                    idle.pop(0)()
    for job in idle:
        job()

    for c in range(FF_CHUNKS):
        ff.drain(c)
        ag_drain(1 + c, last_rows(c))
    for c in range(FF_CHUNKS):
        put(c).wait()


def fetching(size, paired, *refs):
    count = 15
    theirs, out_ref, mine, sem = refs[:count], refs[count], refs[count + 1 : 2 * count + 1], refs[-1]

    def fetch(i):
        return pltpu.make_async_copy(theirs[i], mine[i], sem.at[i])

    for i in [*range(1, count), 0]:
        fetch(i).start()

    def arrived(some):
        for i in some:
            fetch(i).wait()

    kernel(size, paired, arrived, *mine, out_ref, *refs[2 * count + 1 : -1])


def sum_buffers(count, chips, share, cols):
    return (
        pltpu.VMEM((count, chips, share, cols), F32),
        pltpu.VMEM((count, chips, share, cols), BF16),
        pltpu.VMEM((count, chips, share, cols), BF16),
        pltpu.VMEM((count, 6, share // 2, cols), BF16),
        pltpu.VMEM((count, 6, share // 2, cols), BF16),
        pltpu.SemaphoreType.DMA((count, 2)),
        pltpu.SemaphoreType.DMA((count, 4)),
    )


def shards(size, *args):
    (x, gain1, wq, wk, wv, first, second, bias, extra, hgain, wo, gain2, wg, wu, wd) = args
    n, tp = size["fs"], size["tp"]
    paired = size["grp"] % 2 == 0
    rows, wide = x.shape
    depth, keyw = wq.shape
    valw, ffw = wv.shape[1], wg.shape[1]
    share, chips, blocks = rows // tp, tp // 2, rows // BLOCK
    cols = wide // FF_CHUNKS
    padded = -(-wd.shape[0] // 8) * 8
    sems = pltpu.SemaphoreType.DMA
    vmem = pltpu.VMEM
    steps = n // 2
    given = (
        x, gain1.reshape(1, -1), wq, wk, wv, first.T, second, bias.reshape(1, -1), extra.T,
        hgain.reshape(1, -1), wo, gain2.reshape(1, -1), wg, wu, wd,
    )
    out = pl.pallas_call(
        functools.partial(fetching, size, paired),
        out_shape=jax.ShapeDtypeStruct((tp, share, wide), BF16),
        in_specs=[pl.BlockSpec(memory_space=pltpu.HBM)] * len(given),
        out_specs=pl.BlockSpec(memory_space=pltpu.HBM),
        scratch_shapes=[vmem(a.shape, a.dtype) for a in given] + [
            vmem((n, depth, 2 * keyw + valw), BF16),
            vmem((n, wo.shape[0], wide), BF16),
            vmem((n, depth, 2 * ffw), BF16),
            vmem((FF_CHUNKS, n, padded, cols), BF16),
            vmem((rows, wide), BF16),
            vmem((rows, 1), F32),
            vmem((2, 4, rows, keyw), F32),
            vmem((2, blocks, 8, keyw), F32),
            vmem((rows, keyw), BF16),
            vmem((rows, keyw), BF16),
            vmem((rows, valw), BF16),
            vmem((rows, valw), F32),
            vmem((blocks, valw, keyw), F32),
            vmem((blocks, valw, keyw), F32),
            vmem((blocks, valw, 2 * keyw), BF16),
            vmem((blocks, BLOCK, valw), BF16),
            vmem((n * wo.shape[0], wide), BF16),
            vmem((ffw, n * padded), BF16),
            vmem((tp, share, n * padded), BF16),
            vmem((rows, 2 * ffw), F32),
            sum_buffers(MIX_CHUNKS, chips, share, wide // MIX_CHUNKS),
            sum_buffers(FF_CHUNKS, chips, share, cols),
            vmem((share, wide), BF16),
            vmem((tp, share, wide), BF16),
            vmem((tp, share, wide), BF16),
            sems((2 + len(GU_ROWS) + len(DN_SPLIT), 2)),
            sems((2 + len(GU_ROWS) + len(DN_SPLIT), 2, steps)),
            sems((2 + len(GU_ROWS),)),
            sems((2 + len(GU_ROWS),)),
            sems((1 + FF_CHUNKS,)),
            sems((1 + FF_CHUNKS, 5)),
            sems((FF_CHUNKS,)),
            sems((len(given),)),
        ],
        compiler_params=pltpu.CompilerParams(
            collective_id=0, has_side_effects=True, vmem_limit_bytes=VMEM_MIB * 1024 * 1024
        ),
        name="layer",
    )(*given)
    return out.reshape(rows, wide)


def solution(mesh):
    placed = (
        P(("grp", "fs"), None),
        P(),
        P("fs", "tp"),
        P("fs", "tp"),
        P("fs", "tp"),
        P(),
        P(None, "tp"),
        P("tp"),
        P(("grp", "fs"), "tp"),
        P(),
        P(("tp", "fs"), None),
        P(),
        P("fs", "tp"),
        P("fs", "tp"),
        P(("tp", "fs"), None),
    )
    return jax.shard_map(
        functools.partial(shards, dict(mesh.shape)),
        mesh=mesh, in_specs=placed, out_specs=P(("grp", "fs"), None), check_vma=False,
    )
```

```python
import functools

import jax
import jax.numpy as jnp
from jax import lax
from jax.experimental import pallas as pl
from jax.experimental.pallas import tpu as pltpu
from jax.sharding import PartitionSpec as P

MESH = pl.DeviceIdType.MESH
BLOCK = 64
LANES = 128
GATE = 16.0
EPS = 1e-06
MIX_CHUNKS = 2
FF_CHUNKS = 2
VMEM_MIB = 60
GU_ROWS = (16, 16)
DN_SPLIT = (1, 1)
START = {"qkv": 0, "out": 0, "gu0": 7, "gu1": 8, "dn0": 9, "dn1": 11}
PUMP = (1, 1, 1, 1, 2, 1, 1, 1, 1)
F32 = jnp.float32
BF16 = jnp.bfloat16


def mm(a, b):
    return lax.dot_general(a, b, (((1,), (0,)), ((), ())), preferred_element_type=F32)


def mm_nt(a, b):
    return lax.dot_general(a, b, (((1,), (1,)), ((), ())), preferred_element_type=F32)


def mm_tn(a, b):
    return lax.dot_general(a, b, (((0,), (0,)), ((), ())), preferred_element_type=F32)


def iota(shape, dim):
    return lax.broadcasted_iota(jnp.int32, shape, dim)


def scaled_rows(wide, gain):
    return wide * lax.rsqrt(jnp.mean(wide * wide, axis=-1, keepdims=True) + EPS) * gain


def kernel(
    size, paired, arrived,
    x_ref, gain1_ref, wq_ref, wk_ref, wv_ref, first_ref, second_ref, bias_ref, extra_ref,
    hgain_ref, wo_ref, gain2_ref, wg_ref, wu_ref, wd_ref,
    out_ref,
    g_qkv, g_out, g_gu, g_dn,
    normed, extra_col, decs, ends, qs, ks, vs, inside, ups_f, ups_b, car, headed, wout,
    place, hid, wide_gu, mix_bufs, ff_bufs, own_res, full2, full3,
    z_send, z_recv, y_send, y_recv, ag_send, ag_recv, out_sem,
):
    n, tp = size["fs"], size["tp"]
    chips = tp // 2
    far = chips // 2
    grp, me, t = lax.axis_index("grp"), lax.axis_index("fs"), lax.axis_index("tp")
    chip, core = t // 2, t % 2
    half = grp % 2 if paired else 0
    up_z, down_z = lax.rem(me + 1, n), lax.rem(me + n - 1, n)
    twin = grp + 1 - 2 * (grp % 2)
    mate = t + 1 - 2 * core
    right, left = lax.rem(t + 2, tp), lax.rem(t + tp - 2, tp)
    rows = x_ref.shape[0]
    share = rows // tp
    blocks = rows // BLOCK
    keyw = wq_ref.shape[1]
    valw = wv_ref.shape[1]
    wide = x_ref.shape[1]
    mix_cols, cols = wide // MIX_CHUNKS, wide // FF_CHUNKS
    ffw = wg_ref.shape[1]
    whole = ffw // LANES * LANES
    rest = ffw - whole

    barrier = pltpu.get_barrier_semaphore()
    up_two, down_two = lax.rem(me + 2, n), lax.rem(me + n - 2, n)
    friends = [{"fs": z} for z in (up_z, down_z, up_two, down_two)]
    friends += [{"tp": mate}, {"tp": right}, {"tp": left}]
    if paired:
        friends.append({"grp": twin})
    for friend in friends:
        pl.semaphore_signal(barrier, inc=1, device_id=friend, device_id_type=MESH)

    arrived(range(1, 15))
    g_qkv[me, :, 0:keyw] = wq_ref[...]
    g_qkv[me, :, keyw : 2 * keyw] = wk_ref[...]
    g_qkv[me, :, 2 * keyw :] = wv_ref[...]
    g_out[me] = wo_ref[...]
    g_gu[me, :, 0:whole] = wg_ref[:, 0:whole]
    g_gu[me, :, whole : 2 * whole] = wu_ref[:, 0:whole]
    g_gu[me, :, 2 * whole :] = jnp.concatenate([wg_ref[:, whole:], wu_ref[:, whole:]], axis=1)
    dn_rows = wd_ref.shape[0]
    for c in range(FF_CHUNKS):
        g_dn[c, me] = jnp.zeros(g_dn.shape[2:], BF16)
        g_dn[c, me, 0:dn_rows, :] = wd_ref[:, c * cols : (c + 1) * cols]
    eye = iota((BLOCK, BLOCK), 0) == iota((BLOCK, BLOCK), 1)
    for b in range(blocks):
        span = slice(b * BLOCK, (b + 1) * BLOCK)
        extra_col[span, :] = jnp.sum(jnp.where(eye, extra_ref[:, span], 0.0), axis=1, keepdims=True)
    pl.semaphore_wait(barrier, len(friends))

    depth = wq_ref.shape[0]
    lot = depth // 2 if paired else depth

    def part_of(ref, first, count):
        return lambda slots: ref.at[slots, pl.ds(pl.multiple_of(half * lot + first, 8), count), :]

    QKV, OUT = "qkv", "out"
    out_cols = wide // 2 if paired else wide

    def out_part(slots):
        return g_out.at[slots, :, pl.ds(pl.multiple_of(half * out_cols, LANES), out_cols)]

    views = {QKV: part_of(g_qkv, 0, lot), OUT: out_part}
    strided = (QKV, OUT)
    GU, DN = [], []
    first = 0
    for k, count in enumerate(GU_ROWS):
        count = count * lot // sum(GU_ROWS)
        GU.append(f"gu{k}")
        views[GU[k]] = part_of(g_gu, first, count)
        first += count
    first = 0
    for k, count in enumerate(DN_SPLIT):
        views[f"dn{k}"] = lambda slots, first=first, count=count: g_dn.at[pl.ds(first, count), slots]
        DN += [f"dn{k}"] * count
        first += count
    number = {p: i for i, p in enumerate(views)}
    crossing = {p: i for i, p in enumerate([QKV, OUT] + GU)} if paired else {}
    hops = (n // 2, n - 1 - n // 2)

    def z_copy(p, way, s, view=None):
        if view is None:
            view = views[p](lax.rem(me - s + n, n) if way == 0 else lax.rem(me + s, n))
        return pltpu.make_async_remote_copy(
            src_ref=view, dst_ref=view,
            send_sem=z_send.at[number[p], way], recv_sem=z_recv.at[number[p], way, s],
            device_id={"fs": up_z if way == 0 else down_z}, device_id_type=MESH,
        )

    def y_copy(p, view):
        return pltpu.make_async_remote_copy(
            src_ref=view, dst_ref=view,
            send_sem=y_send.at[crossing[p]], recv_sem=y_recv.at[crossing[p]],
            device_id={"grp": twin}, device_id_type=MESH,
        )

    def cross(p, way, s):
        slot = lax.rem(me - s - 1 + n, n) if way == 0 else lax.rem(me + s + 1, n)
        y_copy(p, views[p](slot)).start()

    def step(p, s, ways=(0, 1), arrive=True, leave=True):
        for way in ways:
            if arrive:
                z_copy(p, way, s - 1).wait_recv()
            if leave:
                z_copy(p, way, s).start()
            if arrive and p in crossing:
                cross(p, way, s - 1)

    def away(way, distance):
        return lax.rem(me - distance + n, n) if way == 0 else lax.rem(me + distance, n)

    def far_copy(p, way, distance, two):
        view = views[p](away(way, distance))
        to = (up_two if two else up_z) if way == 0 else (down_two if two else down_z)
        return pltpu.make_async_remote_copy(
            src_ref=view, dst_ref=view, send_sem=z_send.at[number[p], way],
            recv_sem=z_recv.at[number[p], way, distance + (1 if two else 0)],
            device_id={"fs": to}, device_id_type=MESH,
        )

    def far_step(p, j):
        known = isinstance(j, int)
        for way in (0, 1):
            for distance in (2 * j - 1, 2 * j):
                if not known or distance <= hops[way]:
                    z_copy(p, way, distance - 1).wait_recv()
                    if not known or distance <= hops[way] - 2:
                        far_copy(p, way, distance, True).start()
                    if p in crossing:
                        cross(p, way, distance - 1)

    def at(p, s):
        if p in strided:
            if s > 0:
                far_step(p, s)
            else:
                for way in (0, 1):
                    far_copy(p, way, 0, False).start()
                    far_copy(p, way, 0, True).start()
            return
        for way in (0, 1):
            if s <= hops[way]:
                step(p, s, (way,), arrive=s > 0, leave=s < hops[way])

    def y_arrived(p):
        if p in crossing:
            y_copy(p, views[p](pl.ds(0, n - 1))).wait_recv()

    starts = {p: START[p] for p in views}
    order = sorted(views, key=lambda p: (starts[p], number[p]))
    clock = [0]
    final = {p: n // 4 if p in strided else n // 2 for p in views}
    even = {p: n // 4 - 1 if p in strided else hops[1] for p in views}

    def pump(count=1):
        for _ in range(count):
            tick = clock[0]
            for p in order:
                if 0 <= tick - starts[p] <= final[p]:
                    at(p, tick - starts[p])
            clock[0] += 1

    def complete(p):
        while clock[0] <= starts[p] + final[p]:
            pump()

    def glide(count, beside):
        end = clock[0] + count
        while clock[0] < end:
            tick = clock[0]
            inner = [p for p in order if 1 <= tick - starts[p] < even[p]]
            length = 0
            while tick + length < end and all(
                (1 <= tick + length - starts[p] < even[p])
                if p in inner
                else not 0 <= tick + length - starts[p] <= final[p]
                for p in order
            ):
                length += 1
            if length < 3:
                pump()
                beside(tick)
                continue

            def body(now, carry, inner=inner):
                for p in inner:
                    (far_step if p in strided else step)(p, now - starts[p])
                beside(now)
                return carry

            lax.fori_loop(tick, tick + length, body, 0)
            clock[0] += length

    def drain(p):
        for way in (0, 1):
            z_copy(p, way, 0, views[p](pl.ds(0, hops[way]))).wait_send()
        if p in crossing:
            y_copy(p, views[p](pl.ds(0, n - 1))).wait_send()

    low = iota((BLOCK, BLOCK), 0) >= iota((BLOCK, BLOCK), 1)
    high = iota((BLOCK, BLOCK), 0) <= iota((BLOCK, BLOCK), 1)

    def prepare(b):
        span = pl.ds(pl.multiple_of(b * BLOCK, BLOCK), BLOCK)
        tidy = scaled_rows(x_ref[span, :].astype(F32), gain1_ref[...]).astype(BF16)
        normed[span, :] = tidy
        lowrank = mm_nt(tidy, first_ref[...]).astype(BF16)
        logits = mm(lowrank, second_ref[...]) + bias_ref[...]
        logsig = jnp.minimum(logits, 0.0) - jnp.log1p(jnp.exp(-jnp.abs(logits)))
        dec = logsig / GATE + extra_col[span, :]
        one = dec.astype(BF16)
        left_over = dec - one.astype(F32)
        two = left_over.astype(BF16)
        three = (left_over - two.astype(F32)).astype(BF16)
        terms = jnp.concatenate([one, two, three], axis=1)
        for way, mask in ((0, low), (1, high)):
            sums = mm(jnp.where(mask, 1.0, 0.0).astype(BF16), terms)
            run = sums[:, 0:keyw] + sums[:, keyw : 2 * keyw] + sums[:, 2 * keyw :]
            mid_row = BLOCK // 2 - 1 if way == 0 else BLOCK // 2
            end_row = BLOCK - 1 if way == 0 else 0
            middle = run[mid_row : mid_row + 1, :]
            closing = run[end_row : end_row + 1, :]
            decs[way, 0, span, :] = jnp.exp(run)
            decs[way, 1, span, :] = jnp.exp(run - middle)
            decs[way, 2, span, :] = jnp.exp(middle - run)
            decs[way, 3, span, :] = jnp.exp(closing - run)
            ends[way, b] = jnp.broadcast_to(jnp.exp(closing), (8, keyw))

    pump()
    arrived([0])

    place_rows = iota(place.shape, 0)
    place_cols = iota(place.shape, 1)
    padded = g_dn.shape[2]
    place[...] = jnp.where(
        (place_rows // dn_rows == place_cols // padded)
        & (place_rows % dn_rows == place_cols % padded),
        1.0,
        0.0,
    ).astype(BF16)
    glide(starts[QKV] + final[QKV] + 1 - clock[0], lambda tick: None)
    y_arrived(QKV)
    for lo in range(0, blocks, blocks // 2):

        @pl.loop(lo, lo + blocks // 2)
        def _(b):
            prepare(b)

        pump()

    def project(lo, hi):
        return mm(normed[...], g_qkv[:, :, lo:hi].reshape(n * depth, hi - lo)).astype(BF16)

    both = project(0, 2 * keyw)
    qs[...] = both[:, 0:keyw]
    ks[...] = both[:, keyw:]
    pump(PUMP[0])
    vs[...] = project(2 * keyw, 2 * keyw + valw)

    for b in range(blocks):
        span = slice(b * BLOCK, (b + 1) * BLOCK)
        q, k, v = qs[span, :].astype(F32), ks[span, :].astype(F32), vs[span, :]
        scores = 0.0
        for way, mask in ((0, low), (1, high)):
            pair = mm_nt(
                (q * decs[way, 1, span, :]).astype(BF16), (k * decs[way, 2, span, :]).astype(BF16)
            )
            scores = scores + jnp.where(mask, pair, 0.0)
            (ups_f, ups_b)[way][b] = mm_tn(v, (k * decs[way, 3, span, :]).astype(BF16))
        inside[span, :] = mm(scores.astype(BF16), v)
        if b % 4 == 3:
            pump(PUMP[1])
    for way, ups, blocks_in_turn in ((0, ups_f, range(blocks)), (1, ups_b, range(blocks - 1, -1, -1))):
        state = jnp.zeros((valw, keyw), F32)
        for b in blocks_in_turn:
            car[b, :, way * keyw : (way + 1) * keyw] = state.astype(BF16)
            state = state * ends[way, b, 0:1, :] + ups[b]
    complete(OUT)
    y_arrived(OUT)
    wout[...] = g_out[...].astype(F32).reshape(wout.shape).astype(BF16)
    for b in range(blocks):
        span = slice(b * BLOCK, (b + 1) * BLOCK)
        q = qs[span, :].astype(F32)
        reach = jnp.concatenate(
            [(q * decs[0, 0, span, :]).astype(BF16), (q * decs[1, 0, span, :]).astype(BF16)], axis=1
        )
        mixed = inside[span, :] + mm_nt(reach, car[b])
        headed[b] = scaled_rows(mixed, hgain_ref[...]).astype(BF16)
    pump(PUMP[2])

    low_rows, high_rows = slice(0, share // 2), slice(share // 2, share)

    def chip_rows(ref, which):
        return jnp.concatenate([ref[2 * i + which] for i in range(chips)], axis=0)

    ahead, behind = lax.rem(chip + 1, chips), lax.rem(chip + chips - 1, chips)
    across = lax.rem(chip + far, chips)

    class Sums:
        def __init__(self, bufs):
            self.bufs = bufs
            self.own, self.sent, self.got, self.tx, self.rx = bufs[:5]

        def copy(self, src, dst, sent, got, to):
            return pltpu.make_async_remote_copy(
                src_ref=src, dst_ref=dst, send_sem=sent, recv_sem=got,
                device_id={"tp": to}, device_id_type=MESH,
            )

        def ring(self, q, k):
            return self.copy(
                self.tx.at[q, k], self.rx.at[q, k], self.bufs[5].at[q, 1],
                self.bufs[6].at[q, {0: 1, 3: 2}.get(k, 3)], right if k < 3 else left,
            )

        def rings(self, q, count):
            some = pl.ds(0, count)
            return self.copy(
                self.tx.at[q, some], self.rx.at[q, some], self.bufs[5].at[q, 1],
                self.bufs[6].at[q, 3], right,
            )

        def pair(self, q):
            return self.copy(
                self.sent.at[q], self.got.at[q], self.bufs[5].at[q, 0], self.bufs[6].at[q, 0], mate
            )

        def multiply(self, q, source, weight):
            other = mm(chip_rows(source, 1 - core), weight)
            self.sent[q] = other.astype(BF16).reshape(self.sent.shape[1:])
            self.pair(q).start()
            self.own[q] = mm(chip_rows(source, core), weight).reshape(self.own.shape[1:])

        def of(self, q, which, span):
            return self.own[q, which, span, :] + self.got[q, which, span, :].astype(F32)

        def send_off(self, q):
            self.pair(q).wait_recv()
            self.tx[q, 0] = self.of(q, across, low_rows).astype(BF16)
            self.tx[q, 3] = self.of(q, across, high_rows).astype(BF16)
            self.ring(q, 0).start()
            self.ring(q, 3).start()
            self.tx[q, 1] = self.of(q, ahead, high_rows).astype(BF16)
            self.tx[q, 4] = self.of(q, behind, low_rows).astype(BF16)
            self.ring(q, 1).start()
            self.ring(q, 4).start()

        def relay(self, q):
            self.ring(q, 0).wait_recv()
            self.tx[q, 2] = (self.of(q, ahead, low_rows) + self.rx[q, 0].astype(F32)).astype(BF16)
            self.ring(q, 2).start()
            self.ring(q, 3).wait_recv()
            self.tx[q, 5] = (self.of(q, behind, high_rows) + self.rx[q, 3].astype(F32)).astype(BF16)
            self.ring(q, 5).start()

        def finish(self, q):
            self.rings(q, 4).wait_recv()
            top = self.of(q, chip, low_rows) + self.rx[q, 2].astype(F32) + self.rx[q, 4].astype(F32)
            end = self.of(q, chip, high_rows) + self.rx[q, 1].astype(F32) + self.rx[q, 5].astype(F32)
            return jnp.concatenate([top, end], axis=0)

        def drain(self, q):
            self.pair(q).wait_send()
            self.rings(q, 6).wait_send()

    mix, ff = Sums(mix_bufs), Sums(ff_bufs)

    def ag_copy(a, k, buf):
        opposite = lax.rem(t + 2 * far, tp)
        slot, span, to = [
            (t, None, mate),
            (t, None, right),
            (t, None, left),
            (left, low_rows, right),
            (right, high_rows, left),
            (left, None, mate),
            (right, None, mate),
            (opposite, low_rows, mate),
            (opposite, high_rows, mate),
        ][k]
        view = buf(slot, slice(None) if span is None else span)
        return ag_any(a, view, {1: 0, 2: 1, 3: 2, 4: 3}.get(k, 4), to)

    def ag_any(a, view, got, to):
        return pltpu.make_async_remote_copy(
            src_ref=view, dst_ref=view, send_sem=ag_send.at[a], recv_sem=ag_recv.at[a, got],
            device_id={"tp": to}, device_id_type=MESH,
        )

    def ag_drain(a, buf):
        ag_any(a, buf(pl.ds(0, tp - 1), slice(None)), 0, mate).wait_send()

    def ag_start(a, buf):
        for k in (1, 2, 0):
            ag_copy(a, k, buf).start()

    def ag_relay(a, buf):
        ag_copy(a, 1, buf).wait_recv()
        ag_copy(a, 3, buf).start()
        ag_copy(a, 5, buf).start()
        ag_copy(a, 2, buf).wait_recv()
        ag_copy(a, 4, buf).start()
        ag_copy(a, 6, buf).start()

    def ag_finish(a, buf):
        ag_copy(a, 3, buf).wait_recv()
        ag_copy(a, 7, buf).start()
        ag_copy(a, 4, buf).wait_recv()
        ag_copy(a, 8, buf).start()
        ag_any(a, buf(pl.ds(0, tp // 2), slice(None)), 4, mate).wait_recv()

    def mid_rows(slots, span):
        return full2.at[slots, span, :]

    def last_rows(c):
        return lambda slots, span: full3.at[slots, span, c * cols : (c + 1) * cols]

    for c in range(MIX_CHUNKS):
        mix.multiply(c, headed, wout[:, c * mix_cols : (c + 1) * mix_cols])
    pump(PUMP[3])
    for c in range(MIX_CHUNKS):
        mix.send_off(c)
    pump(PUMP[4])
    mix.relay(0)
    pump(PUMP[5])
    mix.relay(1)
    pump(PUMP[6])
    own_rows = pl.ds(pl.multiple_of(t * share, share), share)
    for c in range(MIX_CHUNKS):
        span = slice(c * mix_cols, (c + 1) * mix_cols)
        own_res[:, span] = (x_ref[own_rows, span].astype(F32) + mix.finish(c)).astype(BF16)
    full2[t] = scaled_rows(own_res[...].astype(F32), gain2_ref[...]).astype(BF16)
    ag_start(0, mid_rows)
    pump(PUMP[7])
    ag_relay(0, mid_rows)
    pump(PUMP[8])
    ag_finish(0, mid_rows)
    for p in GU:
        complete(p)
    for p in GU:
        y_arrived(p)

    normed2 = full2[...].reshape(rows, wide)
    for lo in range(0, 2 * ffw, 2 * LANES):
        hi = min(lo + 2 * LANES, 2 * ffw)
        wide_gu[:, lo:hi] = mm(normed2, g_gu[:, :, lo:hi].reshape(n * depth, hi - lo))
    for i in range(tp):
        span = slice(i * share, (i + 1) * share)
        tail = wide_gu[span, 2 * whole :]
        gate = jnp.concatenate([wide_gu[span, 0:whole], tail[:, 0:rest]], axis=1)
        up = jnp.concatenate([wide_gu[span, whole : 2 * whole], tail[:, rest:]], axis=1)
        hidden = (gate / (1.0 + jnp.exp(-gate)) * up).astype(BF16)
        hid[i] = mm(hidden, place[...]).astype(BF16)
    pump()

    def multiply(c):
        complete(DN[c])
        weight = g_dn[c].astype(F32).reshape(n * padded, cols).astype(BF16)
        ff.multiply(c, hid, weight)

    def finish(c):
        done = own_res[:, c * cols : (c + 1) * cols].astype(F32) + ff.finish(c)
        full3[t, :, c * cols : (c + 1) * cols] = done.astype(BF16)
        ag_start(1 + c, last_rows(c))

    def put(c):
        span = slice(c * cols, (c + 1) * cols)
        return pltpu.make_async_copy(full3.at[:, :, span], out_ref.at[:, :, span], out_sem.at[c])

    def end(c):
        ag_finish(1 + c, last_rows(c))
        put(c).start()

    stages = (multiply, ff.send_off, ff.relay, finish, lambda c: ag_relay(1 + c, last_rows(c)), end)
    idle = [functools.partial(drain, p) for p in order] + [
        functools.partial(mix.drain, c) for c in range(MIX_CHUNKS)
    ] + [functools.partial(ag_drain, 0, mid_rows)]
    for beat in range(FF_CHUNKS + len(stages) - 1):
        for k in reversed(range(len(stages))):
            if 0 <= beat - k < FF_CHUNKS:
                stages[k](beat - k)
        if beat >= FF_CHUNKS:
            for _ in range(3):
                if idle:
                    idle.pop(0)()
    for job in idle:
        job()

    for c in range(FF_CHUNKS):
        ff.drain(c)
        ag_drain(1 + c, last_rows(c))
    for c in range(FF_CHUNKS):
        put(c).wait()


def fetching(size, paired, *refs):
    count = 15
    theirs, out_ref, mine, sem = refs[:count], refs[count], refs[count + 1 : 2 * count + 1], refs[-1]

    def fetch(i):
        return pltpu.make_async_copy(theirs[i], mine[i], sem.at[i])

    for i in [*range(1, count), 0]:
        fetch(i).start()

    def arrived(some):
        for i in some:
            fetch(i).wait()

    kernel(size, paired, arrived, *mine, out_ref, *refs[2 * count + 1 : -1])


def sum_buffers(count, chips, share, cols):
    return (
        pltpu.VMEM((count, chips, share, cols), F32),
        pltpu.VMEM((count, chips, share, cols), BF16),
        pltpu.VMEM((count, chips, share, cols), BF16),
        pltpu.VMEM((count, 6, share // 2, cols), BF16),
        pltpu.VMEM((count, 6, share // 2, cols), BF16),
        pltpu.SemaphoreType.DMA((count, 2)),
        pltpu.SemaphoreType.DMA((count, 4)),
    )


def shards(size, *args):
    (x, gain1, wq, wk, wv, first, second, bias, extra, hgain, wo, gain2, wg, wu, wd) = args
    n, tp = size["fs"], size["tp"]
    paired = size["grp"] % 2 == 0
    rows, wide = x.shape
    depth, keyw = wq.shape
    valw, ffw = wv.shape[1], wg.shape[1]
    share, chips, blocks = rows // tp, tp // 2, rows // BLOCK
    cols = wide // FF_CHUNKS
    padded = -(-wd.shape[0] // 8) * 8
    sems = pltpu.SemaphoreType.DMA
    vmem = pltpu.VMEM
    steps = n // 2
    given = (
        x, gain1.reshape(1, -1), wq, wk, wv, first.T, second, bias.reshape(1, -1), extra.T,
        hgain.reshape(1, -1), wo, gain2.reshape(1, -1), wg, wu, wd,
    )
    out = pl.pallas_call(
        functools.partial(fetching, size, paired),
        out_shape=jax.ShapeDtypeStruct((tp, share, wide), BF16),
        in_specs=[pl.BlockSpec(memory_space=pltpu.HBM)] * len(given),
        out_specs=pl.BlockSpec(memory_space=pltpu.HBM),
        scratch_shapes=[vmem(a.shape, a.dtype) for a in given] + [
            vmem((n, depth, 2 * keyw + valw), BF16),
            vmem((n, wo.shape[0], wide), BF16),
            vmem((n, depth, 2 * ffw), BF16),
            vmem((FF_CHUNKS, n, padded, cols), BF16),
            vmem((rows, wide), BF16),
            vmem((rows, 1), F32),
            vmem((2, 4, rows, keyw), F32),
            vmem((2, blocks, 8, keyw), F32),
            vmem((rows, keyw), BF16),
            vmem((rows, keyw), BF16),
            vmem((rows, valw), BF16),
            vmem((rows, valw), F32),
            vmem((blocks, valw, keyw), F32),
            vmem((blocks, valw, keyw), F32),
            vmem((blocks, valw, 2 * keyw), BF16),
            vmem((blocks, BLOCK, valw), BF16),
            vmem((n * wo.shape[0], wide), BF16),
            vmem((ffw, n * padded), BF16),
            vmem((tp, share, n * padded), BF16),
            vmem((rows, 2 * ffw), F32),
            sum_buffers(MIX_CHUNKS, chips, share, wide // MIX_CHUNKS),
            sum_buffers(FF_CHUNKS, chips, share, cols),
            vmem((share, wide), BF16),
            vmem((tp, share, wide), BF16),
            vmem((tp, share, wide), BF16),
            sems((2 + len(GU_ROWS) + len(DN_SPLIT), 2)),
            sems((2 + len(GU_ROWS) + len(DN_SPLIT), 2, steps)),
            sems((2 + len(GU_ROWS),)),
            sems((2 + len(GU_ROWS),)),
            sems((1 + FF_CHUNKS,)),
            sems((1 + FF_CHUNKS, 5)),
            sems((FF_CHUNKS,)),
            sems((len(given),)),
        ],
        compiler_params=pltpu.CompilerParams(
            collective_id=0, has_side_effects=True, vmem_limit_bytes=VMEM_MIB * 1024 * 1024
        ),
        name="layer",
    )(*given)
    return out.reshape(rows, wide)


def solution(mesh):
    placed = (
        P(("grp", "fs"), None),
        P(),
        P("fs", "tp"),
        P("fs", "tp"),
        P("fs", "tp"),
        P(),
        P(None, "tp"),
        P("tp"),
        P(("grp", "fs"), "tp"),
        P(),
        P(("tp", "fs"), None),
        P(),
        P("fs", "tp"),
        P("fs", "tp"),
        P(("tp", "fs"), None),
    )
    return jax.shard_map(
        functools.partial(shards, dict(mesh.shape)),
        mesh=mesh, in_specs=placed, out_specs=P(("grp", "fs"), None), check_vma=False,
    )
```
